32 devices in a mesh: sp: 8 (over z, y), tp: 4 (over x, core).
Axes of the slice: x: 2, y: 2, z: 4, core: 2. Of those that a mesh axis runs over, the one named last changes fastest.
Arguments:
- tokens: bfloat16 [4096, 2048], P(('sp', 'tp')), may hold values from -6 to 6
- norm_gain: bfloat16 [2048], replicated, may hold values from 0.099609375 to 1.8984375
- proj_x: bfloat16 [2048, 2048], P('sp', 'tp'), may hold values from -0.125 to 0.125
- gate_projection: bfloat16 [2048, 2048], P('sp', 'tp'), may hold values from -0.125 to 0.125
- conv_taps: bfloat16 [4, 2048], P(None, 'tp'), may hold values from -3 to 3
- gate_recur: bfloat16 [8, 256, 256], P('tp'), may hold values from -0.375 to 0.375
- gate_input: bfloat16 [8, 256, 256], P('tp'), may hold values from -0.375 to 0.375
- decay_param: float32 [2048], P('tp'), may hold values from 4 to 25
- decay_shift: float32 [8, 4096], P('tp', 'sp'), may hold values from -1.3 to 0, as said below
- proj_out: bfloat16 [2048, 2048], P('tp', 'sp'), may hold values from -0.125 to 0.125
Outputs:
- mixed_out: bfloat16 [4096, 2048], P(('sp', 'tp'))
The draws below stay inside these ranges and needn't reach their ends.
Inputs may be any that keep to these rules, and one draw needn't show every extreme that they name: `decay_shift`: added log-decays, never positive.
All inputs are finite; a program needn't handle non-finite values.
Results may differ from the reference program's by a relative error of at most 0.015.
Values may be sent and summed in bfloat16 or wider, within the bound.
A program may use at most 128 MiB of HBM per device.

```python
import jax
import jax.numpy as jnp
from jax import lax

D = 2048
WIDTH = 2048
HEAD = 256
CONV = 4
GROUP = 512
SEQ = 4096
N_TP = 4


def draw_decay_param(key, part):
    key_pick, key_slow, key_fast = jax.random.split(jax.random.fold_in(key, 11), 3)
    fast_share = 0.5
    picked = jax.random.uniform(key_pick, (WIDTH,), jnp.float32) < fast_share
    slow_rate = jnp.exp(jax.random.uniform(key_slow, (WIDTH,), jnp.float32, jnp.log(0.1), jnp.log(0.6))) / (8.0 * SEQ)
    fast_rate = jnp.exp(jax.random.uniform(key_fast, (WIDTH,), jnp.float32, jnp.log(0.0025), jnp.log(0.0083)))
    chosen = jnp.where(picked, fast_rate, slow_rate)
    return -jnp.log(jnp.expm1(chosen))


def draw_decay_shift(key, part):
    key_base, key_where, key_size = jax.random.split(jax.random.fold_in(key, 23), 3)
    head_count = WIDTH // HEAD
    block_count = SEQ // GROUP
    base = jnp.exp(jax.random.uniform(key_base, (block_count,), jnp.float32, jnp.log(0.05), jnp.log(0.3))) / SEQ
    starting_rows = jnp.repeat(base, GROUP)
    target_slots = jax.random.randint(key_where, (head_count, 2), 0, SEQ)
    segment_sizes = jax.random.uniform(key_size, (head_count, 2), jnp.float32, 0.22, 0.6)
    token_offsets = jnp.arange(SEQ)
    token_runs = jnp.sum(jnp.where(token_offsets[None, None, :] == target_slots[:, :, None], segment_sizes[:, :, None], 0.0), axis=1)
    return -(starting_rows[None, :] + token_runs)


def shard_levels(own_key, extent, pieces, least, largest):
    factor_of = 1.0
    for position, blocks in pieces:
        draws = jax.random.uniform(jax.random.fold_in(jax.random.fold_in(own_key, 6), position), (blocks,), jnp.float32, least / len(pieces), largest / len(pieces))
        factor_of = factor_of * jnp.repeat(jnp.exp(draws), extent[position] // blocks).reshape((-1,) + (1,) * (len(extent) - 1 - position))
    return factor_of


def normal_values(stream_key, extent, spread, limit, cuts=(), kind=jnp.bfloat16):
    result = spread * jax.random.normal(stream_key, extent, jnp.float32)
    if cuts:
        result = result * shard_levels(stream_key, extent, cuts, -0.22, 0.18)
    return jnp.clip(result, -limit, limit).astype(kind)


def setup_inputs(seed: int = 0) -> dict:
    key_list = jax.random.split(jax.random.key(seed), 11)
    return {
        "tokens": normal_values(key_list[0], (SEQ, D), 1.0, 6.0, ((0, 32),)),
        "norm_gain": jnp.clip(1.0 + 0.18 * jax.random.normal(key_list[1], (D,), jnp.float32), 0.099609375, 1.8984375).astype(jnp.bfloat16),
        "proj_x": normal_values(key_list[2], (D, WIDTH), D ** -0.5, 0.125, ((0, 8), (1, 4))),
        "gate_projection": normal_values(key_list[3], (D, WIDTH), D ** -0.5, 0.125, ((0, 8), (1, 4))),
        "conv_taps": normal_values(key_list[4], (CONV, WIDTH), CONV ** -0.5, 3.0, ((1, 4),)),
        "gate_recur": normal_values(key_list[5], (WIDTH // HEAD, HEAD, HEAD), HEAD ** -0.5, 0.375, ((0, 4),)),
        "gate_input": normal_values(key_list[6], (WIDTH // HEAD, HEAD, HEAD), HEAD ** -0.5, 0.375, ((0, 4),)),
        "decay_param": draw_decay_param(jax.random.fold_in(key_list[10], 71), 0),
        "decay_shift": draw_decay_shift(jax.random.fold_in(key_list[10], 71), 0),
        "proj_out": normal_values(key_list[9], (WIDTH, D), WIDTH ** -0.5, 0.125, ((0, 4), (1, 8))),
    }


def rms_norm(values, norm_gain):
    floats = values.astype(jnp.float32)
    scaled = floats * lax.rsqrt(lax.optimization_barrier(jnp.mean(floats * floats, axis=-1, keepdims=True)) + 1e-06)
    return (scaled * norm_gain.astype(jnp.float32)).astype(jnp.bfloat16)

def combine_pair(earlier, later):
    return (earlier[0] * later[0], later[0] * earlier[1] + later[1])

def reference(tokens, norm_gain, proj_x, gate_projection, conv_taps, gate_recur, gate_input, decay_param, decay_shift, proj_out):
    block_count = SEQ // GROUP
    head_count = WIDTH // HEAD
    channel_block = WIDTH // N_TP
    token_blocks = tokens.reshape(block_count, GROUP, D)
    shift_blocks = jnp.transpose(decay_shift.reshape(head_count, block_count, GROUP), (1, 2, 0))
    decay_rate = jax.nn.softplus(-decay_param.astype(jnp.float32)).reshape(head_count, HEAD)

    def advance(carried, inputs):
        state_now, tail_rows = carried
        block_tokens, block_shift = inputs
        normed = rms_norm(block_tokens, norm_gain)
        branch = jnp.dot(normed, proj_x, preferred_element_type=jnp.float32).astype(jnp.bfloat16)
        gating = jnp.dot(normed, gate_projection, preferred_element_type=jnp.float32).astype(jnp.bfloat16)
        extended = jnp.concatenate([tail_rows, branch], axis=0)
        conv_sum = jnp.zeros((GROUP, WIDTH), jnp.float32)
        for tap_index in range(CONV):
            conv_sum = conv_sum + extended[tap_index:tap_index + GROUP].astype(jnp.float32) * conv_taps[tap_index].astype(jnp.float32)
        conved = conv_sum.astype(jnp.bfloat16)
        grouped = conved.reshape(GROUP, head_count, HEAD).astype(jnp.float32)
        recur = jax.nn.sigmoid(jnp.einsum('thi,hij->thj', grouped, gate_recur.astype(jnp.float32)))
        inlet = jax.nn.sigmoid(jnp.einsum('thi,hij->thj', grouped, gate_input.astype(jnp.float32)))
        log_decay = (-8.0 * recur * decay_rate[None] + block_shift[:, :, None]).reshape(GROUP, WIDTH)
        decay = jnp.exp(log_decay)
        drive = jnp.sqrt(-jnp.expm1(2.0 * log_decay)) * inlet.reshape(GROUP, WIDTH) * conved.astype(jnp.float32)
        drive = drive.at[0].add(decay[0] * state_now)
        states = lax.associative_scan(combine_pair, (decay, drive), axis=0)[1]
        mixed = (states * jax.nn.gelu(gating.astype(jnp.float32))).astype(jnp.bfloat16)
        total = jnp.zeros((GROUP, D), jnp.float32)
        for block_index in range(N_TP):
            lower = block_index * channel_block
            partial_out = jnp.dot(mixed[:, lower:lower + channel_block], proj_out[lower:lower + channel_block], preferred_element_type=jnp.float32).astype(jnp.bfloat16)
            total = total + lax.optimization_barrier(partial_out).astype(jnp.float32)
        return ((states[GROUP - 1], branch[GROUP - CONV + 1:]), total.astype(jnp.bfloat16))
    initial = (jnp.zeros((WIDTH,), jnp.float32), jnp.zeros((CONV - 1, WIDTH), jnp.bfloat16))
    unused, output_values = lax.scan(advance, initial, (token_blocks, shift_blocks))
    return output_values.reshape(SEQ, D)
```

```python
import functools

import jax
import jax.numpy as jnp
from jax import lax
from jax.experimental import pallas as pl
from jax.experimental.pallas import tpu as pltpu
from jax.sharding import PartitionSpec as P

HEAD = 256
CONV = 4


def shifted(block, axis, distance):
    devices = range(lax.axis_size(axis))
    route = [(i - distance, i) for i in devices if i - distance in devices]
    return lax.ppermute(block, axis, route)


def carried_in(array, axis, combine, identity):
    size, index = (lax.axis_size(axis), lax.axis_index(axis))
    everything = jax.tree.map(lambda part: lax.all_gather(part, axis), array)
    start = jax.tree.map(
        lambda part, zero: jnp.broadcast_to(jnp.asarray(zero, part.dtype), part.shape),
        array,
        identity,
    )

    def turn(k, before):
        reached = k < index
        new = combine(before, jax.tree.map(lambda part: part[k], everything))
        return jax.tree.map(lambda a, b: jnp.where(reached, a, b), new, before)

    return lax.fori_loop(0, size, turn, start)


def rms_norm(values, norm_gain):
    floats = values.astype(jnp.float32)
    scaled = floats * lax.rsqrt(jnp.mean(floats * floats, axis=-1, keepdims=True) + 1e-06)
    return (scaled * norm_gain.astype(jnp.float32)).astype(jnp.bfloat16)


def combine_pair(earlier, later):
    return (earlier[0] * later[0], later[0] * earlier[1] + later[1])


def on_device(
    tokens,
    norm_gain,
    proj_x,
    gate_projection,
    conv_taps,
    gate_recur,
    gate_input,
    decay_param,
    decay_shift,
    proj_out,
):
    normed = rms_norm(tokens, norm_gain)
    full_x, full_gate = (
        lax.all_gather(proj_x, "sp", axis=0, tiled=True),
        lax.all_gather(gate_projection, "sp", axis=0, tiled=True),
    )
    local_width = proj_x.shape[1]
    piece = lax.all_gather(normed, "tp", axis=0, tiled=True)
    branch_piece = jnp.dot(piece, full_x, preferred_element_type=jnp.float32).astype(jnp.bfloat16)
    gating_piece = jnp.dot(piece, full_gate, preferred_element_type=jnp.float32).astype(
        jnp.bfloat16
    )
    joined = jnp.concatenate([branch_piece, gating_piece], axis=1)
    branch = joined[:, :local_width]
    gating = joined[:, local_width:]
    row_count = branch.shape[0]
    tail_rows = shifted(branch[row_count - CONV + 1 :], "sp", 1)
    extended = jnp.concatenate([tail_rows, branch], axis=0)
    conv_sum = jnp.zeros((row_count, local_width), jnp.float32)
    for tap_index in range(CONV):
        conv_sum = conv_sum + extended[tap_index : tap_index + row_count].astype(
            jnp.float32
        ) * conv_taps[tap_index].astype(jnp.float32)
    conved = conv_sum.astype(jnp.bfloat16)
    head_count = gate_recur.shape[0]
    grouped = conved.reshape(row_count, head_count, HEAD)
    recur = jax.nn.sigmoid(
        jnp.einsum("thi,hij->thj", grouped, gate_recur, preferred_element_type=jnp.float32)
    )
    inlet = jax.nn.sigmoid(
        jnp.einsum("thi,hij->thj", grouped, gate_input, preferred_element_type=jnp.float32)
    )
    decay_rate = jax.nn.softplus(-decay_param).reshape(head_count, HEAD)
    log_decay = (-8.0 * recur * decay_rate[None] + jnp.transpose(decay_shift)[:, :, None]).reshape(
        row_count, local_width
    )
    decay = jnp.exp(log_decay)
    drive = (
        jnp.sqrt(-jnp.expm1(2.0 * log_decay))
        * inlet.reshape(row_count, local_width)
        * conved.astype(jnp.float32)
    )
    identity = (jnp.ones((local_width,), jnp.float32), jnp.zeros((local_width,), jnp.float32))
    cumulative, local_state = lax.associative_scan(combine_pair, (decay, drive), axis=0)
    carried = carried_in(
        (cumulative[row_count - 1], local_state[row_count - 1]), "sp", combine_pair, identity
    )
    states = local_state + cumulative * carried[1][None, :]
    mixed = (states * jax.nn.gelu(gating.astype(jnp.float32))).astype(jnp.bfloat16)
    out_cols = lax.all_gather(proj_out, "sp", axis=1, tiled=True)
    return lax.psum_scatter(
        jnp.dot(mixed, out_cols, preferred_element_type=jnp.float32).astype(jnp.bfloat16),
        "tp",
        scatter_dimension=0,
        tiled=True,
    )


MESH = pl.DeviceIdType.MESH


def fused(
    nz, tok, gain, wx, wg, taps, gr, gi, dp, ds, wo, out,
    xb, wxb, wgb, wob, bf, hs, cum, shc, dsb, mx, cs, cr, carry, psend, keep, precv, sb, acc, rb,
    w_send, w_recv, y_send, t_send, t_recv, m_send, m_recv, c_send, c_recv, p_send, p_recv, r_send, r_recv,
):
    sp, tp = lax.axis_index("sp"), lax.axis_index("tp")
    z, y = sp // 2, sp % 2
    x, c = tp // 2, tp % 2
    rows, width = tok.shape
    krows, half = wx.shape[0], wx.shape[1] // 2
    ocols = wo.shape[1]
    f32, bf16 = jnp.float32, jnp.bfloat16
    y2, x2, c2 = 1 - y, 1 - x, 1 - c
    dev_c, dev_x = (sp, 2 * x + c2), (sp, 2 * x2 + c)
    dev_y, dev_xy = (2 * z + y2, tp), (2 * z + y2, 2 * x2 + c)

    def line(zz):
        return (2 * zz + y, tp)

    def remote(src, dst, ssem, rsem, device):
        return pltpu.make_async_remote_copy(
            src_ref=src, dst_ref=dst, send_sem=ssem, recv_sem=rsem, device_id=device, device_id_type=MESH
        )

    barrier = pltpu.get_barrier_semaphore()
    for device in (dev_c, dev_x, dev_y, dev_xy):
        pl.semaphore_signal(barrier, inc=1, device_id=device, device_id_type=MESH)
    for k in range(1, nz):
        pl.semaphore_signal(barrier, inc=1, device_id=line((z + k) % nz), device_id_type=MESH)

    slot0 = y * 4 + tp
    for part in range(4):
        step = rows // 4
        rs = pl.ds(part * step, step)
        v = tok[rs, :].astype(f32)
        v = v * lax.rsqrt(jnp.mean(v * v, axis=-1, keepdims=True) + 1e-06)
        xb[slot0, rs, :] = (v * gain[...].astype(f32)).astype(bf16)

    bufs = (wxb, wgb, wob)

    def piece(w, zz, yy):
        return bufs[w].at[pl.ds(pl.multiple_of((2 * zz + yy) * half, half), half), :]

    def source(w, yy):
        if w == 2:
            return wo.at[pl.ds(pl.multiple_of(yy * half, half), half), :]
        return (wx, wg)[w].at[:, pl.ds(pl.multiple_of(yy * half, half), half)]

    def to_y(w):
        return remote(source(w, y2), piece(w, z, y), y_send.at[w], w_recv.at[w, z, y], dev_y)

    def from_y(w):
        return remote(source(w, y2), piece(w, z, y2), y_send.at[w], w_recv.at[w, z, y2], dev_y)

    def along(w, zz, yy, direction, src=None):
        device = line(z + 1) if direction == 0 else line(z - 1)
        return remote(
            piece(w, zz, yy) if src is None else src, piece(w, zz, yy),
            w_send.at[w, zz, yy, direction], w_recv.at[w, zz, yy], device,
        )

    def send_both(w, yy, src=None):
        @pl.when(z + 1 < nz)
        def _():
            along(w, z, yy, 0, src).start()

        @pl.when(z > 0)
        def _():
            along(w, z, yy, 1, src).start()

    def own(w):
        send_both(w, y, source(w, y))
        piece(w, z, y)[...] = source(w, y)[...]
        from_y(w).wait_recv()
        send_both(w, y2)

    near = jnp.minimum(z, nz - 1 - z)

    def origin(u):
        side = (z - (u + 1) // 2) if u % 2 else (z + u // 2)
        outer = jnp.where(2 * z < nz, u, nz - 1 - u)
        return jnp.where(u <= 2 * near, side, outer)

    def arrive(w, u):
        zz = origin(u)
        for yy in (y, y2):
            along(w, zz, yy, 0).wait_recv()

            @pl.when(jnp.logical_and(zz < z, z + 1 < nz))
            def _():
                along(w, zz, yy, 0).start()

            @pl.when(jnp.logical_and(zz > z, z > 0))
            def _():
                along(w, zz, yy, 1).start()

    def slot(yy, xx, cc):
        return yy * 4 + xx * 2 + cc

    cut = rows * 3 // 4
    top, low = pl.ds(0, cut), pl.ds(cut, rows - cut)

    def token(src, dst, s, r, device):
        return remote(src, dst, t_send.at[s], t_recv.at[r], device)

    def block(yy, xx, cc):
        return xb.at[slot(yy, xx, cc)]

    def same(ref, s, r, device):
        return token(ref, ref, s, r, device)

    pl.semaphore_wait(barrier, 4 + nz - 1)
    to_y(0).start()
    same(block(y, x, c), 1, 0, dev_x).start()
    same(block(y, x, c), 2, 1, dev_y).start()
    same(block(y, x, c), 0, 4, dev_c).start()
    shift_copy = remote(ds, dsb, m_send.at[1], m_recv.at[1], dev_y)
    shift_copy.start()
    to_y(1).start()
    own(0)

    shift_copy.wait_recv()
    mine = jnp.where(y == 0, ds[0:1, :], ds[1:2, :])
    theirs = jnp.where(y == 0, dsb[0:1, :], dsb[1:2, :])
    first = jnp.where(y == 0, mine, theirs)
    second = jnp.where(y == 0, theirs, mine)
    for b in range(8):
        row = (first, second)[b // 4][:, (b % 4) * rows : (b % 4 + 1) * rows]
        shc[b] = jnp.broadcast_to(row, (rows, rows)).T

    arrive(0, 1)
    for u in range(2, nz - 1):
        arrive(0, u)

    @pl.when(near > 0)
    def _():
        arrive(0, nz - 1)

    same(block(y, x2, c), 1, 0, dev_x).wait_recv()
    same(block(y, x2, c).at[low], 3, 3, dev_y).start()
    same(block(y, x2, c), 4, 5, dev_c).start()
    same(block(y2, x, c), 2, 1, dev_y).wait_recv()
    same(block(y2, x, c).at[top], 5, 2, dev_x).start()
    same(block(y2, x, c), 6, 6, dev_c).start()
    to_y(2).start()

    @pl.when(near == 0)
    def _():
        arrive(0, nz - 1)

    own(1)
    same(block(y2, x2, c).at[top], 5, 2, dev_x).wait_recv()
    same(block(y2, x2, c).at[low], 3, 3, dev_y).wait_recv()
    same(block(y2, x2, c), 7, 7, dev_c).start()
    same(block(y, x, c2), 0, 4, dev_c).wait_recv()
    same(block(y, x2, c2), 4, 5, dev_c).wait_recv()
    same(block(y2, x, c2), 6, 6, dev_c).wait_recv()
    same(block(y2, x2, c2), 7, 7, dev_c).wait_recv()

    @pl.when(z == 0)
    def _():
        bf[0:8, :] = jnp.zeros((8, half), f32)

    @pl.loop(0, 8)
    def _(b):
        v = jnp.dot(xb[b], wxb[...], preferred_element_type=f32)
        bf[pl.ds(pl.multiple_of(8 + b * rows, 8), rows), :] = v.astype(bf16).astype(f32)

    def tail(device):
        return remote(bf.at[pl.ds(8 * rows, 8), :], bf.at[pl.ds(0, 8), :], m_send.at[0], m_recv.at[0], device)

    @pl.when(z + 1 < nz)
    def _():
        tail(line(z + 1)).start()

    arrive(1, 1)

    @pl.when(z > 0)
    def _():
        tail(line(z - 1)).wait_recv()

    lanes = pl.ds(pl.multiple_of(y * half, half), half)
    tap = taps[:, lanes].astype(f32)
    minus = -dp[:, lanes]
    rate = jnp.maximum(minus, 0.0) + jnp.log1p(jnp.exp(-jnp.abs(minus)))
    index = lax.broadcasted_iota(jnp.int32, (rows, half), 0)

    def shift_rows(v, s, fill):
        if s < 8:
            return jnp.where(index >= s, pltpu.roll(v, s, 0), fill)
        return jnp.concatenate([jnp.full((s, half), fill, f32), v[: rows - s]], axis=0)

    def recurrence(b, before):
        window = bf[pl.ds(pl.multiple_of(b * rows, 8), rows + 8), :]
        total = jnp.zeros((rows, half), f32)
        for k in range(CONV):
            lo = 8 - CONV + 1 + k
            total = total + window[lo : lo + rows] * tap[k : k + 1]
        conved = total.astype(bf16)
        recur = jax.nn.sigmoid(jnp.dot(conved, gr[y], preferred_element_type=f32))
        inlet = jax.nn.sigmoid(jnp.dot(conved, gi[y], preferred_element_type=f32))
        shift = shc[b]
        shift = jnp.concatenate([shift] * (half // rows), axis=1)
        log_decay = -8.0 * recur * rate + shift
        a = jnp.exp(log_decay)
        t = 2.0 * log_decay
        series = 1.0 + t * (1.0 / 9.0)
        for k in range(8, 1, -1):
            series = 1.0 + t * (1.0 / k) * series
        lost = jnp.where(t > -0.5, -t * series, 1.0 - a * a)
        h = jnp.sqrt(lost) * inlet * conved.astype(f32)
        s = 1
        while s < rows:
            h = a * shift_rows(h, s, 0.0) + h
            a = a * shift_rows(a, s, 1.0)
            s *= 2
        h = h + a * before[1]
        a = a * before[0]
        hs[b] = h
        cum[b] = a
        return (a[rows - 1 :], h[rows - 1 :])

    state = (jnp.ones((1, half), f32), jnp.zeros((1, half), f32))
    state = lax.fori_loop(0, 4, recurrence, state)
    for u in range(2, nz - 1):
        arrive(1, u)
    state = lax.fori_loop(4, 8, recurrence, state)
    cs[0:8, :] = jnp.broadcast_to(state[0], (8, half))
    cs[8:16, :] = jnp.broadcast_to(state[1], (8, half))

    def carries(k, zz, device):
        return remote(cs, cr.at[zz], c_send.at[k], c_recv.at[zz], device)

    for k in range(1, nz):
        @pl.when(z + k < nz)
        def _():
            carries(k, z, line(z + k)).start()

    arrive(1, nz - 1)
    own(2)

    @pl.when(z + 1 < nz)
    def _():
        tail(line(z + 1)).wait_send()

    @pl.loop(0, 8)
    def _(b):
        v = jnp.dot(xb[b], wgb[...], preferred_element_type=f32).astype(bf16).astype(f32)
        inner = 0.7978845608028654 * (v + 0.044715 * (v * v * v))
        bf[pl.ds(pl.multiple_of(8 + b * rows, 8), rows), :] = 0.5 * v * (1.0 + jnp.tanh(inner))

    carry[...] = jnp.zeros((8, half), f32)
    for k in range(nz - 1):
        @pl.when(k < z)
        def _():
            carries(0, k, dev_y).wait_recv()
            carry[...] = cr[k, 0:8, :] * carry[...] + cr[k, 8:16, :]

    @pl.loop(0, 8)
    def _(b):
        gate = bf[pl.ds(pl.multiple_of(8 + b * rows, 8), rows), :]
        mx[b] = ((hs[b] + cum[b] * carry[0:1, :]) * gate).astype(bf16)

    def partial(u):
        zz = origin(u)

        @pl.loop(0, 4)
        def _(q):
            for yy in range(2):
                cols = pl.ds(yy * ocols, ocols)
                weights = piece(2, zz, yy)[...]
                psend[u, q, :, cols] = jnp.dot(mx[2 * q + c2], weights, preferred_element_type=f32).astype(bf16)

        exchange(u).start()

        @pl.loop(0, 4)
        def _(q):
            for yy in range(2):
                cols = pl.ds(yy * ocols, ocols)
                weights = piece(2, zz, yy)[...]
                keep[u, q, :, cols] = jnp.dot(mx[2 * q + c], weights, preferred_element_type=f32)

    def exchange(u):
        return remote(psend.at[u], precv.at[u], p_send.at[u], p_recv.at[u], dev_c)

    def spread(u, r):
        return remote(sb.at[u, r], rb.at[u, r], r_send.at[u, r], r_recv.at[u, r], (dev_x, dev_y, dev_xy)[r])

    def pair_sum(u):
        exchange(u).wait_recv()
        for r, q in enumerate((2 * y + x2, 2 * y2 + x, 2 * y2 + x2)):
            sb[u, r] = (keep[u, q] + precv[u, q].astype(f32)).astype(bf16)
            spread(u, r).start()
        q = 2 * y + x
        acc[u] = keep[u, q] + precv[u, q].astype(f32)

    def finish(u):
        total = acc[u]
        for r in range(3):
            spread(u, r).wait_recv()
            total = total + rb[u, r].astype(f32)
        out[:, pl.ds(pl.multiple_of(origin(u) * 2 * ocols, ocols), 2 * ocols)] = total.astype(bf16)

    for u in range(nz):
        if u:
            arrive(2, u)
        partial(u)
        if u:
            pair_sum(u - 1)
    for u in range(nz - 2):
        finish(u)
    pair_sum(nz - 1)
    for u in range(max(nz - 2, 0), nz):
        finish(u)

    for w in range(3):
        to_y(w).wait_send()
        for zz in range(nz):
            for yy in range(2):
                @pl.when(jnp.logical_and(zz <= z, z + 1 < nz))
                def _():
                    along(w, zz, yy, 0).wait_send()

                @pl.when(jnp.logical_and(zz >= z, z > 0))
                def _():
                    along(w, zz, yy, 1).wait_send()
    full = block(y, x, c)
    for s, ref in enumerate((full, full, full, full.at[low], full, full.at[top], full, full)):
        same(ref, s, 0, dev_c).wait_send()
    shift_copy.wait_send()

    for k in range(1, nz):
        @pl.when(z + k < nz)
        def _():
            carries(k, z, line(z + k)).wait_send()
    for u in range(nz):
        exchange(u).wait_send()
        for r in range(3):
            spread(u, r).wait_send()


def fused_on_device(
    nz, tokens, norm_gain, proj_x, gate_projection, conv_taps, gate_recur, gate_input, decay_param, decay_shift, proj_out
):
    rows, width = tokens.shape
    half = proj_x.shape[1] // 2
    ocols = proj_out.shape[1]
    bf16, f32 = jnp.bfloat16, jnp.float32
    dma = pltpu.SemaphoreType.DMA
    return pl.pallas_call(
        functools.partial(fused, nz),
        out_shape=jax.ShapeDtypeStruct((rows, width), bf16),
        in_specs=[pl.BlockSpec(memory_space=pltpu.VMEM)] * 10,
        out_specs=pl.BlockSpec(memory_space=pltpu.VMEM),
        scratch_shapes=[
            pltpu.VMEM((8, rows, width), bf16),
            pltpu.VMEM((2 * nz * half, half), bf16),
            pltpu.VMEM((2 * nz * half, half), bf16),
            pltpu.VMEM((2 * nz * half, ocols), bf16),
            pltpu.VMEM((8 * rows + 8, half), f32),
            pltpu.VMEM((8, rows, half), f32),
            pltpu.VMEM((8, rows, half), f32),
            pltpu.VMEM((8, rows, rows), f32),
            pltpu.VMEM(decay_shift.shape, f32),
            pltpu.VMEM((8, rows, half), bf16),
            pltpu.VMEM((16, half), f32),
            pltpu.VMEM((nz, 16, half), f32),
            pltpu.VMEM((8, half), f32),
            pltpu.VMEM((nz, 4, rows, 2 * ocols), bf16),
            pltpu.VMEM((nz, 4, rows, 2 * ocols), f32),
            pltpu.VMEM((nz, 4, rows, 2 * ocols), bf16),
            pltpu.VMEM((nz, 3, rows, 2 * ocols), bf16),
            pltpu.VMEM((nz, rows, 2 * ocols), f32),
            pltpu.VMEM((nz, 3, rows, 2 * ocols), bf16),
            dma((3, nz, 2, 2)), dma((3, nz, 2)), dma((3,)), dma((8,)), dma((8,)), dma((2,)), dma((2,)),
            dma((nz,)), dma((nz,)), dma((nz,)), dma((nz,)), dma((nz, 3)), dma((nz, 3)),
        ],
        compiler_params=pltpu.CompilerParams(
            collective_id=0, has_side_effects=True, vmem_limit_bytes=56 * 1024 * 1024
        ),
    )(
        tokens, norm_gain.reshape(1, width), proj_x, gate_projection, conv_taps, gate_recur, gate_input,
        decay_param.reshape(1, -1), decay_shift, proj_out,
    )


def solution(mesh):
    n_sp, n_tp = mesh.shape["sp"], mesh.shape["tp"]
    in_specs = (
        P(("sp", "tp"), None),
        P(),
        P("sp", "tp"),
        P("sp", "tp"),
        P(None, "tp"),
        P("tp", None, None),
        P("tp", None, None),
        P("tp"),
        P("tp", "sp"),
        P("tp", "sp"),
    )
    out_specs = P(("sp", "tp"), None)
    small = n_tp == 4 and n_sp % 2 == 0 and 4 <= n_sp <= 8

    def body(*args):
        rows, heads, krows, ocols = args[0].shape[0], args[5].shape[0], args[2].shape[0], args[9].shape[1]
        fits = heads == 2 and krows == HEAD and ocols == HEAD and args[8].shape[1] == 4 * rows and rows == HEAD // 2
        return fused_on_device(n_sp // 2, *args) if small and fits else on_device(*args)

    return jax.shard_map(
        body, mesh=mesh, in_specs=in_specs, out_specs=out_specs, check_vma=False
    )
```

```python
import functools

import jax
import jax.numpy as jnp
from jax import lax
from jax.experimental import pallas as pl
from jax.experimental.pallas import tpu as pltpu
from jax.sharding import PartitionSpec as P

HEAD = 256
CONV = 4


def shifted(block, axis, distance):
    devices = range(lax.axis_size(axis))
    route = [(i - distance, i) for i in devices if i - distance in devices]
    return lax.ppermute(block, axis, route)


def carried_in(array, axis, combine, identity):
    size, index = (lax.axis_size(axis), lax.axis_index(axis))
    everything = jax.tree.map(lambda part: lax.all_gather(part, axis), array)
    start = jax.tree.map(
        lambda part, zero: jnp.broadcast_to(jnp.asarray(zero, part.dtype), part.shape),
        array,
        identity,
    )

    def turn(k, before):
        reached = k < index
        new = combine(before, jax.tree.map(lambda part: part[k], everything))
        return jax.tree.map(lambda a, b: jnp.where(reached, a, b), new, before)

    return lax.fori_loop(0, size, turn, start)


def rms_norm(values, norm_gain):
    floats = values.astype(jnp.float32)
    scaled = floats * lax.rsqrt(jnp.mean(floats * floats, axis=-1, keepdims=True) + 1e-06)
    return (scaled * norm_gain.astype(jnp.float32)).astype(jnp.bfloat16)


def combine_pair(earlier, later):
    return (earlier[0] * later[0], later[0] * earlier[1] + later[1])


def on_device(
    tokens,
    norm_gain,
    proj_x,
    gate_projection,
    conv_taps,
    gate_recur,
    gate_input,
    decay_param,
    decay_shift,
    proj_out,
):
    normed = rms_norm(tokens, norm_gain)
    full_x, full_gate = (
        lax.all_gather(proj_x, "sp", axis=0, tiled=True),
        lax.all_gather(gate_projection, "sp", axis=0, tiled=True),
    )
    local_width = proj_x.shape[1]
    piece = lax.all_gather(normed, "tp", axis=0, tiled=True)
    branch_piece = jnp.dot(piece, full_x, preferred_element_type=jnp.float32).astype(jnp.bfloat16)
    gating_piece = jnp.dot(piece, full_gate, preferred_element_type=jnp.float32).astype(
        jnp.bfloat16
    )
    joined = jnp.concatenate([branch_piece, gating_piece], axis=1)
    branch = joined[:, :local_width]
    gating = joined[:, local_width:]
    row_count = branch.shape[0]
    tail_rows = shifted(branch[row_count - CONV + 1 :], "sp", 1)
    extended = jnp.concatenate([tail_rows, branch], axis=0)
    conv_sum = jnp.zeros((row_count, local_width), jnp.float32)
    for tap_index in range(CONV):
        conv_sum = conv_sum + extended[tap_index : tap_index + row_count].astype(
            jnp.float32
        ) * conv_taps[tap_index].astype(jnp.float32)
    conved = conv_sum.astype(jnp.bfloat16)
    head_count = gate_recur.shape[0]
    grouped = conved.reshape(row_count, head_count, HEAD)
    recur = jax.nn.sigmoid(
        jnp.einsum("thi,hij->thj", grouped, gate_recur, preferred_element_type=jnp.float32)
    )
    inlet = jax.nn.sigmoid(
        jnp.einsum("thi,hij->thj", grouped, gate_input, preferred_element_type=jnp.float32)
    )
    decay_rate = jax.nn.softplus(-decay_param).reshape(head_count, HEAD)
    log_decay = (-8.0 * recur * decay_rate[None] + jnp.transpose(decay_shift)[:, :, None]).reshape(
        row_count, local_width
    )
    decay = jnp.exp(log_decay)
    drive = (
        jnp.sqrt(-jnp.expm1(2.0 * log_decay))
        * inlet.reshape(row_count, local_width)
        * conved.astype(jnp.float32)
    )
    identity = (jnp.ones((local_width,), jnp.float32), jnp.zeros((local_width,), jnp.float32))
    cumulative, local_state = lax.associative_scan(combine_pair, (decay, drive), axis=0)
    carried = carried_in(
        (cumulative[row_count - 1], local_state[row_count - 1]), "sp", combine_pair, identity
    )
    states = local_state + cumulative * carried[1][None, :]
    mixed = (states * jax.nn.gelu(gating.astype(jnp.float32))).astype(jnp.bfloat16)
    out_cols = lax.all_gather(proj_out, "sp", axis=1, tiled=True)
    return lax.psum_scatter(
        jnp.dot(mixed, out_cols, preferred_element_type=jnp.float32).astype(jnp.bfloat16),
        "tp",
        scatter_dimension=0,
        tiled=True,
    )


MESH = pl.DeviceIdType.MESH


def fused(
    nz, tok, gain, wx, wg, taps, gr, gi, dp, ds, wo, out,
    xb, wxb, wgb, wob, bf, hs, cum, shc, dsb, mx, cs, cr, carry, psend, keep, precv, sb, acc, rb,
    w_send, w_recv, y_send, t_send, t_recv, m_send, m_recv, c_send, c_recv, p_send, p_recv, r_send, r_recv,
):
    sp, tp = lax.axis_index("sp"), lax.axis_index("tp")
    z, y = sp // 2, sp % 2
    x, c = tp // 2, tp % 2
    rows, width = tok.shape
    krows, half = wx.shape[0], wx.shape[1] // 2
    ocols = wo.shape[1]
    f32, bf16 = jnp.float32, jnp.bfloat16
    y2, x2, c2 = 1 - y, 1 - x, 1 - c
    dev_c, dev_x = (sp, 2 * x + c2), (sp, 2 * x2 + c)
    dev_y, dev_xy = (2 * z + y2, tp), (2 * z + y2, 2 * x2 + c)

    def line(zz):
        return (2 * zz + y, tp)

    def remote(src, dst, ssem, rsem, device):
        return pltpu.make_async_remote_copy(
            src_ref=src, dst_ref=dst, send_sem=ssem, recv_sem=rsem, device_id=device, device_id_type=MESH
        )

    barrier = pltpu.get_barrier_semaphore()
    for device in (dev_c, dev_x, dev_y, dev_xy):
        pl.semaphore_signal(barrier, inc=1, device_id=device, device_id_type=MESH)
    for k in range(1, nz):
        pl.semaphore_signal(barrier, inc=1, device_id=line((z + k) % nz), device_id_type=MESH)

    slot0 = y * 4 + tp
    for part in range(4):
        step = rows // 4
        rs = pl.ds(part * step, step)
        v = tok[rs, :].astype(f32)
        v = v * lax.rsqrt(jnp.mean(v * v, axis=-1, keepdims=True) + 1e-06)
        xb[slot0, rs, :] = (v * gain[...].astype(f32)).astype(bf16)

    bufs = (wxb, wgb, wob)

    def piece(w, zz, yy):
        return bufs[w].at[pl.ds(pl.multiple_of((2 * zz + yy) * half, half), half), :]

    def source(w, yy):
        if w == 2:
            return wo.at[pl.ds(pl.multiple_of(yy * half, half), half), :]
        return (wx, wg)[w].at[:, pl.ds(pl.multiple_of(yy * half, half), half)]

    def to_y(w):
        return remote(source(w, y2), piece(w, z, y), y_send.at[w], w_recv.at[w, z, y], dev_y)

    def from_y(w):
        return remote(source(w, y2), piece(w, z, y2), y_send.at[w], w_recv.at[w, z, y2], dev_y)

    def along(w, zz, yy, direction, src=None):
        device = line(z + 1) if direction == 0 else line(z - 1)
        return remote(
            piece(w, zz, yy) if src is None else src, piece(w, zz, yy),
            w_send.at[w, zz, yy, direction], w_recv.at[w, zz, yy], device,
        )

    def send_both(w, yy, src=None):
        @pl.when(z + 1 < nz)
        def _():
            along(w, z, yy, 0, src).start()

        @pl.when(z > 0)
        def _():
            along(w, z, yy, 1, src).start()

    def own(w):
        send_both(w, y, source(w, y))
        piece(w, z, y)[...] = source(w, y)[...]
        from_y(w).wait_recv()
        send_both(w, y2)

    near = jnp.minimum(z, nz - 1 - z)

    def origin(u):
        side = (z - (u + 1) // 2) if u % 2 else (z + u // 2)
        outer = jnp.where(2 * z < nz, u, nz - 1 - u)
        return jnp.where(u <= 2 * near, side, outer)

    def arrive(w, u):
        zz = origin(u)
        for yy in (y, y2):
            along(w, zz, yy, 0).wait_recv()

            @pl.when(jnp.logical_and(zz < z, z + 1 < nz))
            def _():
                along(w, zz, yy, 0).start()

            @pl.when(jnp.logical_and(zz > z, z > 0))
            def _():
                along(w, zz, yy, 1).start()

    def slot(yy, xx, cc):
        return yy * 4 + xx * 2 + cc

    cut = rows * 3 // 4
    top, low = pl.ds(0, cut), pl.ds(cut, rows - cut)

    def token(src, dst, s, r, device):
        return remote(src, dst, t_send.at[s], t_recv.at[r], device)

    def block(yy, xx, cc):
        return xb.at[slot(yy, xx, cc)]

    def same(ref, s, r, device):
        return token(ref, ref, s, r, device)

    pl.semaphore_wait(barrier, 4 + nz - 1)
    to_y(0).start()
    same(block(y, x, c), 1, 0, dev_x).start()
    same(block(y, x, c), 2, 1, dev_y).start()
    same(block(y, x, c), 0, 4, dev_c).start()
    shift_copy = remote(ds, dsb, m_send.at[1], m_recv.at[1], dev_y)
    shift_copy.start()
    to_y(1).start()
    own(0)

    shift_copy.wait_recv()
    mine = jnp.where(y == 0, ds[0:1, :], ds[1:2, :])
    theirs = jnp.where(y == 0, dsb[0:1, :], dsb[1:2, :])
    first = jnp.where(y == 0, mine, theirs)
    second = jnp.where(y == 0, theirs, mine)
    for b in range(8):
        row = (first, second)[b // 4][:, (b % 4) * rows : (b % 4 + 1) * rows]
        shc[b] = jnp.broadcast_to(row, (rows, rows)).T

    arrive(0, 1)
    for u in range(2, nz - 1):
        arrive(0, u)

    @pl.when(near > 0)
    def _():
        arrive(0, nz - 1)

    same(block(y, x2, c), 1, 0, dev_x).wait_recv()
    same(block(y, x2, c).at[low], 3, 3, dev_y).start()
    same(block(y, x2, c), 4, 5, dev_c).start()
    same(block(y2, x, c), 2, 1, dev_y).wait_recv()
    same(block(y2, x, c).at[top], 5, 2, dev_x).start()
    same(block(y2, x, c), 6, 6, dev_c).start()
    to_y(2).start()

    @pl.when(near == 0)
    def _():
        arrive(0, nz - 1)

    own(1)
    same(block(y, x, c2), 0, 4, dev_c).wait_recv()
    same(block(y, x2, c2), 4, 5, dev_c).wait_recv()

    def project(part):
        v = jnp.dot(xb[pl.ds(4 * part, 4)].reshape(4 * rows, width), wxb[...], preferred_element_type=f32)
        bf[pl.ds(pl.multiple_of(8 + part * 4 * rows, 8), 4 * rows), :] = v.astype(bf16).astype(f32)

    project(y)
    same(block(y2, x2, c).at[top], 5, 2, dev_x).wait_recv()
    same(block(y2, x2, c).at[low], 3, 3, dev_y).wait_recv()
    same(block(y2, x2, c), 7, 7, dev_c).start()
    same(block(y2, x, c2), 6, 6, dev_c).wait_recv()
    same(block(y2, x2, c2), 7, 7, dev_c).wait_recv()

    @pl.when(z == 0)
    def _():
        bf[0:8, :] = jnp.zeros((8, half), f32)

    project(y2)

    def tail(device):
        return remote(bf.at[pl.ds(8 * rows, 8), :], bf.at[pl.ds(0, 8), :], m_send.at[0], m_recv.at[0], device)

    @pl.when(z + 1 < nz)
    def _():
        tail(line(z + 1)).start()

    arrive(1, 1)

    @pl.when(z > 0)
    def _():
        tail(line(z - 1)).wait_recv()

    lanes = pl.ds(pl.multiple_of(y * half, half), half)
    tap = taps[:, lanes].astype(f32)
    minus = -dp[:, lanes]
    rate = jnp.maximum(minus, 0.0) + jnp.log1p(jnp.exp(-jnp.abs(minus)))
    index = lax.broadcasted_iota(jnp.int32, (rows, half), 0)

    def shift_rows(v, s, fill):
        if s < 8:
            return jnp.where(index >= s, pltpu.roll(v, s, 0), fill)
        return jnp.concatenate([jnp.full((s, half), fill, f32), v[: rows - s]], axis=0)

    def recurrence(b, before):
        window = bf[pl.ds(pl.multiple_of(b * rows, 8), rows + 8), :]
        total = jnp.zeros((rows, half), f32)
        for k in range(CONV):
            lo = 8 - CONV + 1 + k
            total = total + window[lo : lo + rows] * tap[k : k + 1]
        conved = total.astype(bf16)
        recur = jax.nn.sigmoid(jnp.dot(conved, gr[y], preferred_element_type=f32))
        inlet = jax.nn.sigmoid(jnp.dot(conved, gi[y], preferred_element_type=f32))
        shift = shc[b]
        shift = jnp.concatenate([shift] * (half // rows), axis=1)
        log_decay = -8.0 * recur * rate + shift
        a = jnp.exp(log_decay)
        t = 2.0 * log_decay
        series = 1.0 + t * (1.0 / 9.0)
        for k in range(8, 1, -1):
            series = 1.0 + t * (1.0 / k) * series
        lost = jnp.where(t > -0.5, -t * series, 1.0 - a * a)
        h = jnp.sqrt(lost) * inlet * conved.astype(f32)
        s = 1
        while s < rows:
            h = a * shift_rows(h, s, 0.0) + h
            a = a * shift_rows(a, s, 1.0)
            s *= 2
        h = h + a * before[1]
        a = a * before[0]
        hs[b] = h
        cum[b] = a
        return (a[rows - 1 :], h[rows - 1 :])

    state = (jnp.ones((1, half), f32), jnp.zeros((1, half), f32))
    state = lax.fori_loop(0, 4, recurrence, state)
    for u in range(2, nz - 1):
        arrive(1, u)
    state = lax.fori_loop(4, 8, recurrence, state)
    cs[0:8, :] = jnp.broadcast_to(state[0], (8, half))
    cs[8:16, :] = jnp.broadcast_to(state[1], (8, half))

    def carries(k, zz, device):
        return remote(cs, cr.at[zz], c_send.at[k], c_recv.at[zz], device)

    for k in range(1, nz):
        @pl.when(z + k < nz)
        def _():
            carries(k, z, line(z + k)).start()

    arrive(1, nz - 1)
    own(2)

    @pl.when(z + 1 < nz)
    def _():
        tail(line(z + 1)).wait_send()

    @pl.loop(0, 2)
    def _(part):
        v = jnp.dot(xb[pl.ds(4 * part, 4)].reshape(4 * rows, width), wgb[...], preferred_element_type=f32)
        bf[pl.ds(pl.multiple_of(8 + part * 4 * rows, 8), 4 * rows), :] = v.astype(bf16).astype(f32)

    @pl.loop(0, 8)
    def _(b):
        v = bf[pl.ds(pl.multiple_of(8 + b * rows, 8), rows), :]
        inner = 0.7978845608028654 * (v + 0.044715 * (v * v * v))
        bf[pl.ds(pl.multiple_of(8 + b * rows, 8), rows), :] = 0.5 * v * (1.0 + jnp.tanh(inner))

    carry[...] = jnp.zeros((8, half), f32)
    for k in range(nz - 1):
        @pl.when(k < z)
        def _():
            carries(0, k, dev_y).wait_recv()
            carry[...] = cr[k, 0:8, :] * carry[...] + cr[k, 8:16, :]

    @pl.loop(0, 8)
    def _(b):
        gate = bf[pl.ds(pl.multiple_of(8 + b * rows, 8), rows), :]
        mx[b % 2, b // 2] = ((hs[b] + cum[b] * carry[0:1, :]) * gate).astype(bf16)

    def partial(u):
        zz = origin(u)

        def product(core, yy):
            values = mx[core].reshape(4 * rows, half)
            return jnp.dot(values, piece(2, zz, yy)[...], preferred_element_type=f32).reshape(4, rows, ocols)

        for yy in range(2):
            psend[u, :, :, yy * ocols : (yy + 1) * ocols] = product(c2, yy).astype(bf16)
        exchange(u).start()
        for yy in range(2):
            keep[u, :, :, yy * ocols : (yy + 1) * ocols] = product(c, yy)

    def exchange(u):
        return remote(psend.at[u], precv.at[u], p_send.at[u], p_recv.at[u], dev_c)

    def spread(u, r):
        return remote(sb.at[u, r], rb.at[u, r], r_send.at[u, r], r_recv.at[u, r], (dev_x, dev_y, dev_xy)[r])

    def pair_sum(u):
        exchange(u).wait_recv()
        for r, q in enumerate((2 * y + x2, 2 * y2 + x, 2 * y2 + x2)):
            sb[u, r] = (keep[u, q] + precv[u, q].astype(f32)).astype(bf16)
            spread(u, r).start()
        q = 2 * y + x
        acc[u] = keep[u, q] + precv[u, q].astype(f32)

    def finish(u):
        total = acc[u]
        for r in range(3):
            spread(u, r).wait_recv()
            total = total + rb[u, r].astype(f32)
        out[:, pl.ds(pl.multiple_of(origin(u) * 2 * ocols, ocols), 2 * ocols)] = total.astype(bf16)

    for u in range(nz):
        if u:
            arrive(2, u)
        partial(u)
        if u:
            pair_sum(u - 1)
    for u in range(nz - 2):
        finish(u)
    pair_sum(nz - 1)
    for u in range(max(nz - 2, 0), nz):
        finish(u)

    for w in range(3):
        to_y(w).wait_send()
        for zz in range(nz):
            for yy in range(2):
                @pl.when(jnp.logical_and(zz <= z, z + 1 < nz))
                def _():
                    along(w, zz, yy, 0).wait_send()

                @pl.when(jnp.logical_and(zz >= z, z > 0))
                def _():
                    along(w, zz, yy, 1).wait_send()
    full = block(y, x, c)
    for s, ref in enumerate((full, full, full, full.at[low], full, full.at[top], full, full)):
        same(ref, s, 0, dev_c).wait_send()
    shift_copy.wait_send()

    for k in range(1, nz):
        @pl.when(z + k < nz)
        def _():
            carries(k, z, line(z + k)).wait_send()
    for u in range(nz):
        exchange(u).wait_send()
        for r in range(3):
            spread(u, r).wait_send()


def fused_on_device(
    nz, tokens, norm_gain, proj_x, gate_projection, conv_taps, gate_recur, gate_input, decay_param, decay_shift, proj_out
):
    rows, width = tokens.shape
    half = proj_x.shape[1] // 2
    ocols = proj_out.shape[1]
    bf16, f32 = jnp.bfloat16, jnp.float32
    dma = pltpu.SemaphoreType.DMA
    return pl.pallas_call(
        functools.partial(fused, nz),
        out_shape=jax.ShapeDtypeStruct((rows, width), bf16),
        in_specs=[pl.BlockSpec(memory_space=pltpu.VMEM)] * 10,
        out_specs=pl.BlockSpec(memory_space=pltpu.VMEM),
        scratch_shapes=[
            pltpu.VMEM((8, rows, width), bf16),
            pltpu.VMEM((2 * nz * half, half), bf16),
            pltpu.VMEM((2 * nz * half, half), bf16),
            pltpu.VMEM((2 * nz * half, ocols), bf16),
            pltpu.VMEM((8 * rows + 8, half), f32),
            pltpu.VMEM((8, rows, half), f32),
            pltpu.VMEM((8, rows, half), f32),
            pltpu.VMEM((8, rows, rows), f32),
            pltpu.VMEM(decay_shift.shape, f32),
            pltpu.VMEM((2, 4, rows, half), bf16),
            pltpu.VMEM((16, half), f32),
            pltpu.VMEM((nz, 16, half), f32),
            pltpu.VMEM((8, half), f32),
            pltpu.VMEM((nz, 4, rows, 2 * ocols), bf16),
            pltpu.VMEM((nz, 4, rows, 2 * ocols), f32),
            pltpu.VMEM((nz, 4, rows, 2 * ocols), bf16),
            pltpu.VMEM((nz, 3, rows, 2 * ocols), bf16),
            pltpu.VMEM((nz, rows, 2 * ocols), f32),
            pltpu.VMEM((nz, 3, rows, 2 * ocols), bf16),
            dma((3, nz, 2, 2)), dma((3, nz, 2)), dma((3,)), dma((8,)), dma((8,)), dma((2,)), dma((2,)),
            dma((nz,)), dma((nz,)), dma((nz,)), dma((nz,)), dma((nz, 3)), dma((nz, 3)),
        ],
        compiler_params=pltpu.CompilerParams(
            collective_id=0, has_side_effects=True, vmem_limit_bytes=56 * 1024 * 1024
        ),
    )(
        tokens, norm_gain.reshape(1, width), proj_x, gate_projection, conv_taps, gate_recur, gate_input,
        decay_param.reshape(1, -1), decay_shift, proj_out,
    )


def solution(mesh):
    n_sp, n_tp = mesh.shape["sp"], mesh.shape["tp"]
    in_specs = (
        P(("sp", "tp"), None),
        P(),
        P("sp", "tp"),
        P("sp", "tp"),
        P(None, "tp"),
        P("tp", None, None),
        P("tp", None, None),
        P("tp"),
        P("tp", "sp"),
        P("tp", "sp"),
    )
    out_specs = P(("sp", "tp"), None)
    small = n_tp == 4 and n_sp % 2 == 0 and 4 <= n_sp <= 8

    def body(*args):
        rows, heads, krows, ocols = args[0].shape[0], args[5].shape[0], args[2].shape[0], args[9].shape[1]
        fits = heads == 2 and krows == HEAD and ocols == HEAD and args[8].shape[1] == 4 * rows and rows == HEAD // 2
        return fused_on_device(n_sp // 2, *args) if small and fits else on_device(*args)

    return jax.shard_map(
        body, mesh=mesh, in_specs=in_specs, out_specs=out_specs, check_vma=False
    )
```
